32 devices in a mesh: fs: 16 (over z, y, x), tp: 2 (over core).
Axes of the slice: x: 2, y: 2, z: 4, core: 2. Of those that a mesh axis runs over, the one named last changes fastest.
Arguments:
- late_input: bfloat16 [2048, 2048], P('fs', 'tp'), may hold values from -6 to 6
- up_weight: bfloat16 [2048, 4096], P('tp', 'fs'), may hold values from -0.125 to 0.125
- down_weight: bfloat16 [4096, 2048], P('fs', 'tp'), may hold values from -0.09375 to 0.09375
- early_input: bfloat16 [2048, 2048], P('fs', 'tp'), may hold values from -6 to 6
- early_pre: bfloat16 [2048, 4096], P('fs'), may hold values from -6 to 6
- cotangent: bfloat16 [2048, 2048], P('fs', 'tp'), may hold values from -6 to 6
- up_sum: float32 [2048, 4096], P('tp', 'fs'), may hold values from -24 to 24
- down_sum: float32 [4096, 2048], P('fs', 'tp'), may hold values from -24 to 24
Outputs:
- late_pre: bfloat16 [2048, 4096], P('fs')
- late_out: bfloat16 [2048, 2048], P('fs', 'tp')
- input_grad: bfloat16 [2048, 2048], P('fs', 'tp')
- up_total: float32 [2048, 4096], P('tp', 'fs')
- down_total: float32 [4096, 2048], P('fs', 'tp')
The draws below stay inside these ranges and needn't reach their ends.
All inputs are finite; a program needn't handle non-finite values.
Results may differ from the reference program's by a relative error of at most 0.025.
Values may be sent and summed in bfloat16 or wider, within the bound.
A program may use at most 128 MiB of HBM per device.

```python
import jax
import jax.numpy as jnp
from jax import lax

D = 2048
FF = 4096
TOKENS = 2048
DBLK = 1024
N_TP = 2


def spiked(drawn, own_key, source, target, parts, factor):
    owner, partner = [(jnp.arange(drawn.shape[axis_at]) // (drawn.shape[axis_at] // parts)).reshape([-1 if axis == axis_at else 1 for axis in range(drawn.ndim)]) for axis_at in (source, target)]
    chosen = jax.random.permutation(own_key, parts)[partner]
    strong = (owner == chosen) | (owner == (partner + parts // 2) % parts)
    return jnp.where(strong, factor * drawn, drawn)


def steps_of(key, shape, split, smallest, largest):
    def one(position, shards_of):
        draws = jax.random.uniform(jax.random.fold_in(jax.random.fold_in(key, 6), position), (shards_of,), jnp.float32, smallest / len(split), largest / len(split))
        return jnp.repeat(jnp.exp(draws), shape[position] // shards_of).reshape((-1,) + (1,) * (len(shape) - position - 1))

    factor_of = one(*split[0])
    for cut in split[1:]:
        factor_of = factor_of * one(*cut)
    return factor_of


def centred(rng, shape, width, reach, split=(), held_as=jnp.bfloat16):
    loudness = steps_of(rng, shape, split, -0.22, 0.18) if split else 1.0
    values = jax.random.normal(rng, shape, jnp.float32) * width * loudness
    return jnp.minimum(jnp.maximum(values, -reach), reach).astype(held_as)


def bell_draw_with(key, shape, width, bound, pieces, heavy, held_as=jnp.bfloat16):
    values = width * jax.random.normal(key, shape, jnp.float32)
    if pieces:
        values = values * steps_of(key, shape, pieces, -0.22, 0.18)
    return jnp.clip(spiked(values, jax.random.fold_in(key, 3), *heavy), -bound, bound).astype(held_as)


def setup_inputs(seed: int = 0) -> dict:
    arg_keys = jax.random.split(jax.random.key(seed), 9)
    return {
        "late_input": centred(arg_keys[0], (TOKENS, D), 1.0, 6.0, ((0, 16), (1, 2))),
        "up_weight": centred(arg_keys[1], (D, FF), D ** -0.5, 0.125, ((0, 2), (1, 16))),
        "down_weight": centred(arg_keys[2], (FF, D), FF ** -0.5, 0.09375, ((0, 16), (1, 2))),
        "early_input": centred(arg_keys[3], (TOKENS, D), 1.0, 6.0, ((0, 16), (1, 2))),
        "early_pre": centred(arg_keys[4], (TOKENS, FF), 1.0, 6.0, ((0, 16),)),
        "cotangent": bell_draw_with(arg_keys[5], (TOKENS, D), 1.0, 6.0, ((0, 16), (1, 2)), (0, 1, 16, 2.0)),
        "up_sum": centred(arg_keys[6], (D, FF), 4.0, 24.0, ((0, 2), (1, 16)), jnp.float32),
        "down_sum": centred(arg_keys[7], (FF, D), 4.0, 24.0, ((0, 16), (1, 2)), jnp.float32),
    }


def block_sum(left, right):
    total = jnp.zeros((left.shape[0], right.shape[1]), jnp.float32)
    for block in range(N_TP):
        lower = block * DBLK
        partial_value = jnp.dot(left[:, lower:lower + DBLK], right[lower:lower + DBLK, :], preferred_element_type=jnp.float32)
        partial_value = lax.optimization_barrier(partial_value.astype(jnp.bfloat16))
        total = total + partial_value.astype(jnp.float32)
    return total


def reference(late_input, up_weight, down_weight, early_input, early_pre, cotangent, up_sum, down_sum):
    late_pre = block_sum(late_input, up_weight).astype(jnp.bfloat16)
    late_hidden = jnp.square(jax.nn.relu(late_pre.astype(jnp.float32))).astype(jnp.bfloat16)
    late_out = jnp.dot(late_hidden, down_weight, preferred_element_type=jnp.float32).astype(jnp.bfloat16)
    early_float = early_pre.astype(jnp.float32)
    early_hidden = jnp.square(jax.nn.relu(early_float)).astype(jnp.bfloat16)
    hidden_grad = block_sum(cotangent, down_weight.T)
    pre_grad = (hidden_grad * 2.0 * jax.nn.relu(early_float)).astype(jnp.bfloat16)
    input_grad = jnp.dot(pre_grad, up_weight.T, preferred_element_type=jnp.float32).astype(jnp.bfloat16)
    up_total = up_sum + jnp.dot(early_input.T, pre_grad, preferred_element_type=jnp.float32)
    down_total = down_sum + jnp.dot(early_hidden.T, cotangent, preferred_element_type=jnp.float32)
    return late_pre, late_out, input_grad, up_total, down_total
```

```python
import jax
import jax.numpy as jnp
from jax import lax
from jax.experimental import pallas as pl
from jax.experimental.pallas import tpu as pltpu
from jax.sharding import PartitionSpec as P

MESH = pl.DeviceIdType.MESH
F32 = jnp.float32
BF16 = jnp.bfloat16


def dot(left, right, lc, rc):
    return lax.dot_general(left, right, (((lc,), (rc,)), ((), ())), preferred_element_type=F32)


def square_relu(value):
    kept = jnp.maximum(value.astype(F32), 0.0)
    return (kept * kept).astype(BF16)


def fused(a, late_in, up_w, down_w, early_in, early_pre, cot, up_sum, down_sum,
          late_pre_o, late_out_o, in_grad_o, up_o, down_o,
          cot_g, late_g, early_g, pre_g, up_g, down_g, gt_s, gt_r, pg, eh, lt_s, lt_r, lp, lh, lp_g,
          part, ig_s, ig_u, ig_d, lo_s, lo_u, lo_d,
          dg_s, dg_x, dg_y, dg_fx, dg_fy, ug_s, ug_x, ug_y, ug_fx, ug_fy,
          ag_ss, ag_rs, w_ss, w_rs, e_ss, e_rs, l_ss, l_rs, t_ss, t_rs, rl_ss, rl_rs, rq_ss, rq_rs):
    side = 4
    half_side = side // 2
    me = lax.axis_index("fs")
    t = lax.axis_index("tp")
    z = me // side
    q = lax.rem(me, side)
    y = q // 2
    x = lax.rem(q, 2)
    qx = y * 2 + (1 - x)
    qy = (1 - y) * 2 + x
    qd = side - 1 - q
    xn = (z * side + qx, t)
    yn = (z * side + qy, t)
    pn = (me, 1 - t)
    above = (lax.rem(me + side, a * side), t)
    below = (lax.rem(me + (a - 1) * side, a * side), t)
    rows = late_in.shape[0]
    ff = up_w.shape[1]
    width = late_in.shape[1]
    cols = ff * side
    step_n = width // side

    barrier = pltpu.get_barrier_semaphore()
    greet = [xn, yn, pn] + [(lax.rem(me + o * side, a * side), t) for o in range(1, a)]
    for device in greet:
        pl.semaphore_signal(barrier, inc=1, device_id=device, device_id_type=MESH)
    pl.semaphore_wait(barrier, len(greet))

    sent = []

    def rc(src, dst, ss, rs, device):
        return pltpu.make_async_remote_copy(
            src_ref=src, dst_ref=dst, send_sem=ss, recv_sem=rs, device_id=device, device_id_type=MESH)

    def send(src, dst, ss, rs, device, cond=None):
        def go():
            rc(src, dst, ss, rs, device).start()

        if cond is None:
            go()
        else:
            pl.when(cond)(go)
        sent.append((cond, rc(src, dst, ss, rs, device)))

    def arrive(dst, ss, rs, cond=None):
        def go():
            rc(dst, dst, ss, rs, pn).wait_recv()

        if cond is None:
            go()
        else:
            pl.when(cond)(go)

    def slot(j):
        return pl.ds(pl.multiple_of(j * rows, rows), rows)

    def line_gather(which, own, buf, d):
        for way in range(2):
            if way == 0:
                j, here, on, device = z - d, z >= d, (z >= d) & (z < a - 1), above
            else:
                j, here, on, device = z + d, z + d < a, (z + d < a) & (z > 0), below
            j = jnp.clip(j, 0, a - 1)
            place = buf.at[slot(j)]
            if d > 0:
                arrive(place, ag_ss.at[which, way, 0], ag_rs.at[which, way, d], here)
            if d < a - 1:
                send(own if d == 0 else place, place, ag_ss.at[which, way, d],
                     ag_rs.at[which, way, d + 1], device, on)

    def half(ref, block, h):
        n = ref.shape[1] // 2
        return ref.at[block, pl.ds(h * n, n)]

    def half2(ref, h):
        n = ref.shape[0] // 2
        return ref.at[pl.ds(h * n, n)]

    def square_send(which, own, buf):
        for h in (0, 1):
            send(half2(own, h), half(buf, q, h), w_ss.at[which, 0, h], w_rs.at[which, 0, h], xn)
            send(half2(own, 1 - h), half(buf, q, 1 - h), w_ss.at[which, 1, 1 - h], w_rs.at[which, 1, 1 - h], yn)

    def square_relay(which, buf):
        arrive(half(buf, qx, 0), w_ss.at[which, 0, 0], w_rs.at[which, 0, 0])
        send(half(buf, qx, 0), half(buf, qx, 0), w_ss.at[which, 1, 2], w_rs.at[which, 1, 2], yn)
        arrive(half(buf, qy, 1), w_ss.at[which, 0, 0], w_rs.at[which, 1, 1])
        send(half(buf, qy, 1), half(buf, qy, 1), w_ss.at[which, 0, 2], w_rs.at[which, 0, 2], xn)

    def square_rest(which, buf):
        arrive(half(buf, qx, 1), w_ss.at[which, 0, 0], w_rs.at[which, 0, 1])
        arrive(half(buf, qy, 0), w_ss.at[which, 0, 0], w_rs.at[which, 1, 0])
        arrive(half(buf, qd, 0), w_ss.at[which, 0, 0], w_rs.at[which, 1, 2])
        arrive(half(buf, qd, 1), w_ss.at[which, 0, 0], w_rs.at[which, 0, 2])

    def square_sum_begin(which, block, staged, first_x, first_y, fin_x, fin_y):
        staged[qd] = block(qd).astype(BF16)
        send(half(staged, qd, 0), first_x, rq_ss.at[which, 0], rq_rs.at[which, 0], xn)
        send(half(staged, qd, 1), first_y, rq_ss.at[which, 1], rq_rs.at[which, 1], yn)
        staged[qx] = block(qx).astype(BF16)
        send(half(staged, qx, 0), half2(fin_x, 0), rq_ss.at[which, 2], rq_rs.at[which, 2], xn)
        staged[qy] = block(qy).astype(BF16)
        send(half(staged, qy, 1), half2(fin_y, 1), rq_ss.at[which, 3], rq_rs.at[which, 3], yn)

    def square_sum_relay(which, staged, first_x, first_y, fin_x, fin_y):
        n = staged.shape[1] // 2
        arrive(first_x, rq_ss.at[which, 0], rq_rs.at[which, 0])
        staged[qy, 0:n] = (staged[qy, 0:n].astype(F32) + first_x[...].astype(F32)).astype(BF16)
        send(half(staged, qy, 0), half2(fin_y, 0), rq_ss.at[which, 4], rq_rs.at[which, 4], yn)
        arrive(first_y, rq_ss.at[which, 0], rq_rs.at[which, 1])
        staged[qx, n:2 * n] = (staged[qx, n:2 * n].astype(F32) + first_y[...].astype(F32)).astype(BF16)
        send(half(staged, qx, 1), half2(fin_x, 1), rq_ss.at[which, 5], rq_rs.at[which, 5], xn)

    def square_sum_end(which, fin_x, fin_y, out):
        arrive(half2(fin_x, 0), rq_ss.at[which, 0], rq_rs.at[which, 2])
        arrive(half2(fin_y, 1), rq_ss.at[which, 0], rq_rs.at[which, 3])
        arrive(half2(fin_y, 0), rq_ss.at[which, 0], rq_rs.at[which, 4])
        arrive(half2(fin_x, 1), rq_ss.at[which, 0], rq_rs.at[which, 5])
        out[...] = out[...] + (fin_x[...].astype(F32) + fin_y[...].astype(F32))

    def line_sum_step(which, staged, from_u, from_d, k):
        for way in range(2):
            if way == 0:
                j, on, more, buf, device = a - k, z < a - k, z > 0, from_u, above
            else:
                j, on, more, buf, device = k - 1, z > k - 1, z < a - 1, from_d, below

            @pl.when(on & more)
            def _(j=j, buf=buf, way=way):
                arrive(buf.at[j], rl_ss.at[which, 0, 0], rl_rs.at[which, way, j])
                staged[j] = (staged[j].astype(F32) + buf[j].astype(F32)).astype(BF16)

            send(staged.at[j], buf.at[j], rl_ss.at[which, way, j], rl_rs.at[which, way, j], device, on)

    def line_sum_end(which, own, from_u, from_d, out):
        @pl.when(z > 0)
        def _():
            arrive(from_u.at[z], rl_ss.at[which, 0, 0], rl_rs.at[which, 0, z])
            own[slot(z)] = own[slot(z)] + from_u[z].astype(F32)

        @pl.when(z < a - 1)
        def _():
            arrive(from_d.at[z], rl_ss.at[which, 0, 0], rl_rs.at[which, 1, z])
            own[slot(z)] = own[slot(z)] + from_d[z].astype(F32)

        out[...] = own[slot(z)].astype(BF16)

    def columns(block, unit):
        return pl.ds(pl.multiple_of(block * unit, unit), unit)

    square_send(1, down_w, down_g)
    line_gather(0, cot, cot_g, 0)
    for o in range(1, a):
        zd = lax.rem(z + o, a)
        for u in range(half_side):
            b = t * half_side + u
            send(early_pre.at[:, columns(zd * side + b, ff)], pre_g.at[b, slot(z)],
                 e_ss.at[0, o, u], e_rs.at[0, o, u], (zd * side + q, t))
    down_g[q] = down_w[...]
    up_g[q] = up_w[...]
    cot_g[slot(z)] = cot[...]
    late_g[slot(z)] = late_in[...]
    early_g[slot(z)] = early_in[...]
    for b in range(side):
        pre_g[b, slot(z)] = early_pre[:, columns(z * side + b, ff)]

    line_gather(0, cot, cot_g, 1)
    square_relay(1, down_g)
    square_send(0, up_w, up_g)
    line_gather(1, late_in, late_g, 0)
    for d in range(2, a):
        line_gather(0, cot, cot_g, d)
    for o in range(1, a):
        zs = lax.rem(z - o + a, a)
        for u in range(half_side):
            b = t * half_side + u
            place = pre_g.at[b, slot(zs)]
            arrive(place, e_ss.at[0, 0, 0], e_rs.at[0, o, u])
            send(place, place, e_ss.at[1, o, u], e_rs.at[1, o, u], pn)
    line_gather(1, late_in, late_g, 1)
    line_gather(2, early_in, early_g, 0)
    square_rest(1, down_g)

    @pl.loop(0, side)
    def _(b):
        gt_s[b] = dot(cot_g[...], down_g[b], 1, 1).astype(BF16)

    send(gt_s, gt_r, t_ss.at[0], t_rs.at[0], pn)
    for d in range(2, a):
        line_gather(1, late_in, late_g, d)
    square_relay(0, up_g)
    for o in range(1, a):
        zs = lax.rem(z - o + a, a)
        for u in range(half_side):
            b = (1 - t) * half_side + u
            arrive(pre_g.at[b, slot(zs)], e_ss.at[0, 0, 0], e_rs.at[1, o, u])

    @pl.loop(0, side)
    def _(b):
        eh[b] = square_relu(pre_g[b])

    square_sum_begin(1, lambda b: dot(eh[b], cot_g[...], 0, 0), dg_s, dg_x, dg_y, dg_fx, dg_fy)
    down_o[...] = down_sum[...] + dot(eh[q], cot_g[...], 0, 0)
    arrive(gt_r, t_ss.at[0], t_rs.at[0])

    @pl.loop(0, side)
    def _(b):
        hidden = gt_s[b].astype(F32) + gt_r[b].astype(F32)
        pg[b] = (hidden * 2.0 * jnp.maximum(pre_g[b].astype(F32), 0.0)).astype(BF16)

    line_gather(2, early_in, early_g, 1)
    square_rest(0, up_g)

    @pl.loop(0, side)
    def _(b):
        lt_s[b] = dot(late_g[...], up_g[b], 1, 0).astype(BF16)

    send(lt_s, lt_r, t_ss.at[1], t_rs.at[1], pn)

    def to_line(which, value, staged):
        @pl.loop(0, side)
        def _(n):
            at = columns(n, step_n)
            part[which, :, at] = value(at)

        for j in range(a):
            staged[j] = part[which, pl.ds(j * rows, rows)].astype(BF16)

    def ig_value(at):
        return sum(dot(pg[b], up_g[b, at, :], 1, 1) for b in range(side))

    to_line(0, ig_value, ig_s)
    line_sum_step(0, ig_s, ig_u, ig_d, 1)
    if a > 2:
        line_gather(2, early_in, early_g, 2)
    square_sum_relay(1, dg_s, dg_x, dg_y, dg_fx, dg_fy)
    arrive(lt_r, t_ss.at[1], t_rs.at[1])

    @pl.loop(0, side)
    def _(b):
        pre = (lt_s[b].astype(F32) + lt_r[b].astype(F32)).astype(BF16)
        lp[b] = pre
        lh[b] = square_relu(pre)

    for o in range(1, a):
        zd = lax.rem(z + o, a)
        for u in range(half_side):
            b = t * half_side + u
            send(lp.at[b, slot(zd)], lp_g.at[:, columns(z * side + b, ff)],
                 l_ss.at[0, o, u], l_rs.at[0, o, u], (zd * side + q, t))
    for b in range(side):
        lp_g[:, columns(z * side + b, ff)] = lp[b, slot(z)]

    def lo_value(at):
        return sum(dot(lh[b], down_g[b, :, at], 1, 0) for b in range(side))

    to_line(1, lo_value, lo_s)
    for k in range(2, a):
        line_sum_step(0, ig_s, ig_u, ig_d, k)
        if k == 2:
            line_sum_step(1, lo_s, lo_u, lo_d, 1)
    for d in range(3, a):
        line_gather(2, early_in, early_g, d)
    square_sum_begin(0, lambda b: dot(early_g[...], pg[b], 0, 0), ug_s, ug_x, ug_y, ug_fx, ug_fy)
    for o in range(1, a):
        zs = lax.rem(z - o + a, a)
        for u in range(half_side):
            place = lp_g.at[:, columns(zs * side + t * half_side + u, ff)]
            arrive(place, l_ss.at[0, 0, 0], l_rs.at[0, o, u])
            send(place, place, l_ss.at[1, o, u], l_rs.at[1, o, u], pn)
    for k in range(2 if a > 2 else 1, a):
        line_sum_step(1, lo_s, lo_u, lo_d, k)
    up_o[...] = up_sum[...] + dot(early_g[...], pg[q], 0, 0)
    square_sum_relay(0, ug_s, ug_x, ug_y, ug_fx, ug_fy)
    square_sum_end(1, dg_fx, dg_fy, down_o)
    line_sum_end(0, part.at[0], ig_u, ig_d, in_grad_o)
    line_sum_end(1, part.at[1], lo_u, lo_d, late_out_o)
    for o in range(1, a):
        zs = lax.rem(z - o + a, a)
        for u in range(half_side):
            place = lp_g.at[:, columns(zs * side + (1 - t) * half_side + u, ff)]
            arrive(place, l_ss.at[0, 0, 0], l_rs.at[1, o, u])
    late_pre_o[...] = lp_g[...]
    square_sum_end(0, ug_fx, ug_fy, up_o)

    for cond, copy in sent:
        if cond is None:
            copy.wait_send()
        else:
            pl.when(cond)(copy.wait_send)


def fused_body(late_input, up_weight, down_weight, early_input, early_pre, cotangent, up_sum, down_sum):
    a = lax.axis_size("fs") // 4
    side = 4
    rows, width = late_input.shape
    ff = up_weight.shape[1]
    tokens, hidden = rows * a, ff * side
    V = pltpu.VMEM
    D = pltpu.SemaphoreType.DMA
    token_block = V((tokens, width), BF16)
    hidden_block = V((side, tokens, ff), BF16)
    line_block = V((a, rows, width), BF16)
    scratch = (
        [token_block] * 3
        + [hidden_block, V((side, width, ff), BF16), V((side, ff, width), BF16)]
        + [hidden_block] * 8
        + [V((rows, hidden * a), BF16), V((2, tokens, width), F32)]
        + [line_block] * 6
        + [V((side, ff, width), BF16)] + [V((ff // 2, width), BF16)] * 2 + [V((ff, width), BF16)] * 2
        + [V((side, width, ff), BF16)] + [V((width // 2, ff), BF16)] * 2 + [V((width, ff), BF16)] * 2
        + [D((3, 2, a)), D((3, 2, a)), D((2, 2, 3)), D((2, 2, 3)), D((2, a, 2)), D((2, a, 2)),
           D((2, a, 2)), D((2, a, 2)), D((2,)), D((2,)), D((2, 2, a)), D((2, 2, a)), D((2, 6)), D((2, 6))]
    )
    flops = 12 * tokens * hidden * width
    return pl.pallas_call(
        lambda *refs: fused(a, *refs),
        out_shape=(
            jax.ShapeDtypeStruct(early_pre.shape, BF16),
            jax.ShapeDtypeStruct(late_input.shape, BF16),
            jax.ShapeDtypeStruct(early_input.shape, BF16),
            jax.ShapeDtypeStruct(up_sum.shape, F32),
            jax.ShapeDtypeStruct(down_sum.shape, F32),
        ),
        in_specs=[pl.BlockSpec(memory_space=pltpu.VMEM)] * 8,
        out_specs=[pl.BlockSpec(memory_space=pltpu.VMEM)] * 5,
        scratch_shapes=scratch,
        compiler_params=pltpu.CompilerParams(
            collective_id=0, has_side_effects=True, vmem_limit_bytes=62 * 1024 * 1024),
        cost_estimate=pl.CostEstimate(flops=flops, bytes_accessed=1 << 24, transcendentals=0),
    )(late_input, up_weight, down_weight, early_input, early_pre, cotangent, up_sum, down_sum)


def contract_rows(left, right):
    return lax.dot_general(
        left, right, (((0,), (0,)), ((), ())), preferred_element_type=jnp.float32
    )


def contract_cols(left, right):
    return lax.dot_general(
        left, right, (((1,), (1,)), ((), ())), preferred_element_type=jnp.float32
    )


def body(late_input, up_weight, down_weight, early_input, early_pre, cotangent, up_sum, down_sum):
    up_gathered = lax.all_gather(up_weight, "fs", axis=1, tiled=True)
    down_gathered = lax.all_gather(down_weight, "fs", axis=0, tiled=True)
    pre_terms = jnp.dot(late_input, up_gathered, preferred_element_type=jnp.float32)
    pre_summed = lax.psum(pre_terms.astype(jnp.bfloat16), "tp")
    late_hidden = jnp.square(jax.nn.relu(pre_summed.astype(jnp.float32))).astype(jnp.bfloat16)
    early_float = early_pre.astype(jnp.float32)
    early_hidden = jnp.square(jax.nn.relu(early_float)).astype(jnp.bfloat16)
    late_out = jnp.dot(late_hidden, down_gathered, preferred_element_type=jnp.float32).astype(
        jnp.bfloat16
    )
    grad_terms = contract_cols(cotangent, down_gathered)
    hidden_grad = lax.psum(grad_terms.astype(jnp.bfloat16), "tp").astype(jnp.float32)
    pre_grad = (hidden_grad * 2.0 * jax.nn.relu(early_float)).astype(jnp.bfloat16)
    input_grad = contract_cols(pre_grad, up_gathered).astype(jnp.bfloat16)
    grad_local, hidden_local = (
        lax.all_to_all(pre_grad, "fs", split_axis=1, concat_axis=0, tiled=True),
        lax.all_to_all(early_hidden, "fs", split_axis=1, concat_axis=0, tiled=True),
    )
    rows = grad_local
    up_grad = contract_rows(lax.all_gather(early_input, "fs", axis=0, tiled=True), rows)
    up_total = up_sum + up_grad
    rows = hidden_local
    down_grad = contract_rows(rows, lax.all_gather(cotangent, "fs", axis=0, tiled=True))
    down_total = down_sum + down_grad
    return (pre_summed, late_out, input_grad, up_total, down_total)


def solution(mesh):
    in_specs = (
        P("fs", "tp"),
        P("tp", "fs"),
        P("fs", "tp"),
        P("fs", "tp"),
        P("fs", None),
        P("fs", "tp"),
        P("tp", "fs"),
        P("fs", "tp"),
    )
    out_specs = (P("fs", None), P("fs", "tp"), P("fs", "tp"), P("tp", "fs"), P("fs", "tp"))
    square_chips = mesh.shape["tp"] == 2 and mesh.shape["fs"] % 4 == 0 and mesh.shape["fs"] >= 8
    chosen = fused_body if square_chips else body
    return jax.shard_map(chosen, mesh=mesh, in_specs=in_specs, out_specs=out_specs, check_vma=False)
```

```python
import jax
import jax.numpy as jnp
from jax import lax
from jax.experimental import pallas as pl
from jax.experimental.pallas import tpu as pltpu
from jax.sharding import PartitionSpec as P

MESH = pl.DeviceIdType.MESH
F32 = jnp.float32
BF16 = jnp.bfloat16


def dot(left, right, lc, rc):
    return lax.dot_general(left, right, (((lc,), (rc,)), ((), ())), preferred_element_type=F32)


def square_relu(value):
    kept = jnp.maximum(value.astype(F32), 0.0)
    return (kept * kept).astype(BF16)


def fused(a, late_in, up_w, down_w, early_in, early_pre, cot,
          late_pre_o, late_out_o, in_grad_o, up_o, down_o,
          cot_g, late_g, early_g, pre_g, up_g, down_g, gt_s, gt_r, pg, eh, lt_s, lt_r, lp, lh, lp_g,
          part, ig_s, ig_u, ig_d, lo_s, lo_u, lo_d,
          dg_s, dg_x, dg_y, dg_fx, dg_fy, ug_s, ug_x, ug_y, ug_fx, ug_fy,
          ag_ss, ag_rs, w_ss, w_rs, e_ss, e_rs, l_ss, l_rs, t_ss, t_rs, rl_ss, rl_rs, rq_ss, rq_rs,
          local_s, down_v, up_v, ig_v, lo_v):
    side = 4
    half_side = side // 2
    me = lax.axis_index("fs")
    t = lax.axis_index("tp")
    z = me // side
    q = lax.rem(me, side)
    y = q // 2
    x = lax.rem(q, 2)
    qx = y * 2 + (1 - x)
    qy = (1 - y) * 2 + x
    qd = side - 1 - q
    xn = (z * side + qx, t)
    yn = (z * side + qy, t)
    pn = (me, 1 - t)
    above = (lax.rem(me + side, a * side), t)
    below = (lax.rem(me + (a - 1) * side, a * side), t)
    rows = late_in.shape[0]
    ff = up_w.shape[1]
    width = late_in.shape[1]
    cols = ff * side
    step_n = width // side

    def begin(src, dst, k):
        copy = pltpu.make_async_copy(src, dst, local_s.at[k])
        copy.start()
        return copy

    own_rows = pl.ds(pl.multiple_of(z * rows, rows), rows)
    own_down = begin(down_w, down_g.at[q], 0)
    own_cot = begin(cot, cot_g.at[own_rows], 1)
    own_up = begin(up_w, up_g.at[q], 2)
    own_late = begin(late_in, late_g.at[own_rows], 3)
    own_early = begin(early_in, early_g.at[own_rows], 4)
    own_pre = [
        begin(early_pre.at[:, pl.ds(pl.multiple_of((z * side + b) * ff, ff), ff)],
              pre_g.at[b, own_rows], 5 + b)
        for b in range(side)
    ]

    barrier = pltpu.get_barrier_semaphore()
    greet = [xn, yn, pn] + [(lax.rem(me + o * side, a * side), t) for o in range(1, a)]
    for device in greet:
        pl.semaphore_signal(barrier, inc=1, device_id=device, device_id_type=MESH)
    pl.semaphore_wait(barrier, len(greet))

    sent = []

    def rc(src, dst, ss, rs, device):
        return pltpu.make_async_remote_copy(
            src_ref=src, dst_ref=dst, send_sem=ss, recv_sem=rs, device_id=device, device_id_type=MESH)

    def send(src, dst, ss, rs, device, cond=None):
        def go():
            rc(src, dst, ss, rs, device).start()

        if cond is None:
            go()
        else:
            pl.when(cond)(go)
        sent.append((cond, rc(src, dst, ss, rs, device)))

    def arrive(dst, ss, rs, cond=None):
        def go():
            rc(dst, dst, ss, rs, pn).wait_recv()

        if cond is None:
            go()
        else:
            pl.when(cond)(go)

    def slot(j):
        return pl.ds(pl.multiple_of(j * rows, rows), rows)

    def line_gather(which, own, buf, d):
        for way in range(2):
            if way == 0:
                j, here, on, device = z - d, z >= d, (z >= d) & (z < a - 1), above
            else:
                j, here, on, device = z + d, z + d < a, (z + d < a) & (z > 0), below
            j = jnp.clip(j, 0, a - 1)
            place = buf.at[slot(j)]
            if d > 0:
                arrive(place, ag_ss.at[which, way, 0], ag_rs.at[which, way, d], here)
            if d < a - 1:
                send(own if d == 0 else place, place, ag_ss.at[which, way, d],
                     ag_rs.at[which, way, d + 1], device, on)

    def half(ref, block, h):
        n = ref.shape[1] // 2
        return ref.at[block, pl.ds(h * n, n)]

    def half2(ref, h):
        n = ref.shape[0] // 2
        return ref.at[pl.ds(h * n, n)]

    def square_send(which, own, buf):
        for h in (0, 1):
            send(half2(own, h), half(buf, q, h), w_ss.at[which, 0, h], w_rs.at[which, 0, h], xn)
            send(half2(own, 1 - h), half(buf, q, 1 - h), w_ss.at[which, 1, 1 - h], w_rs.at[which, 1, 1 - h], yn)

    def square_relay(which, buf):
        arrive(half(buf, qx, 0), w_ss.at[which, 0, 0], w_rs.at[which, 0, 0])
        send(half(buf, qx, 0), half(buf, qx, 0), w_ss.at[which, 1, 2], w_rs.at[which, 1, 2], yn)
        arrive(half(buf, qy, 1), w_ss.at[which, 0, 0], w_rs.at[which, 1, 1])
        send(half(buf, qy, 1), half(buf, qy, 1), w_ss.at[which, 0, 2], w_rs.at[which, 0, 2], xn)

    def square_rest(which, buf):
        arrive(half(buf, qx, 1), w_ss.at[which, 0, 0], w_rs.at[which, 0, 1])
        arrive(half(buf, qy, 0), w_ss.at[which, 0, 0], w_rs.at[which, 1, 0])
        arrive(half(buf, qd, 0), w_ss.at[which, 0, 0], w_rs.at[which, 1, 2])
        arrive(half(buf, qd, 1), w_ss.at[which, 0, 0], w_rs.at[which, 0, 2])

    def square_sum_begin(which, block, staged, first_x, first_y, fin_x, fin_y):
        staged[qd] = block(qd).astype(BF16)
        send(half(staged, qd, 0), first_x, rq_ss.at[which, 0], rq_rs.at[which, 0], xn)
        send(half(staged, qd, 1), first_y, rq_ss.at[which, 1], rq_rs.at[which, 1], yn)
        staged[qx] = block(qx).astype(BF16)
        send(half(staged, qx, 0), half2(fin_x, 0), rq_ss.at[which, 2], rq_rs.at[which, 2], xn)
        staged[qy] = block(qy).astype(BF16)
        send(half(staged, qy, 1), half2(fin_y, 1), rq_ss.at[which, 3], rq_rs.at[which, 3], yn)

    def square_sum_relay(which, staged, first_x, first_y, fin_x, fin_y):
        n = staged.shape[1] // 2
        arrive(first_x, rq_ss.at[which, 0], rq_rs.at[which, 0])
        staged[qy, 0:n] = (staged[qy, 0:n].astype(F32) + first_x[...].astype(F32)).astype(BF16)
        send(half(staged, qy, 0), half2(fin_y, 0), rq_ss.at[which, 4], rq_rs.at[which, 4], yn)
        arrive(first_y, rq_ss.at[which, 0], rq_rs.at[which, 1])
        staged[qx, n:2 * n] = (staged[qx, n:2 * n].astype(F32) + first_y[...].astype(F32)).astype(BF16)
        send(half(staged, qx, 1), half2(fin_x, 1), rq_ss.at[which, 5], rq_rs.at[which, 5], xn)

    def square_sum_end(which, fin_x, fin_y, out):
        arrive(half2(fin_x, 0), rq_ss.at[which, 0], rq_rs.at[which, 2])
        arrive(half2(fin_y, 1), rq_ss.at[which, 0], rq_rs.at[which, 3])
        arrive(half2(fin_y, 0), rq_ss.at[which, 0], rq_rs.at[which, 4])
        arrive(half2(fin_x, 1), rq_ss.at[which, 0], rq_rs.at[which, 5])
        out[...] = out[...] + (fin_x[...].astype(F32) + fin_y[...].astype(F32))

    def line_sum_step(which, staged, from_u, from_d, step):
        for way in range(2):
            if way == 0:
                j, on, more, buf, device = a - 1 + z - step, step >= z, z > 0, from_u, above
            else:
                j, on, more, buf, device = step - (a - 1 - z), step >= a - 1 - z, z < a - 1, from_d, below
            j = jnp.clip(j, 0, a - 1)

            @pl.when(on & more)
            def _(j=j, buf=buf, way=way):
                arrive(buf.at[j], rl_ss.at[which, 0, 0], rl_rs.at[which, way, j])
                staged[j] = (staged[j].astype(F32) + buf[j].astype(F32)).astype(BF16)

            send(staged.at[j], buf.at[j], rl_ss.at[which, way, step], rl_rs.at[which, way, j], device, on)

    def line_sum_end(which, own, from_u, from_d, out):
        @pl.when(z > 0)
        def _():
            arrive(from_u.at[z], rl_ss.at[which, 0, 0], rl_rs.at[which, 0, z])
            own[slot(z)] = own[slot(z)] + from_u[z].astype(F32)

        @pl.when(z < a - 1)
        def _():
            arrive(from_d.at[z], rl_ss.at[which, 0, 0], rl_rs.at[which, 1, z])
            own[slot(z)] = own[slot(z)] + from_d[z].astype(F32)

        out[...] = own[slot(z)].astype(BF16)

    def columns(block, unit):
        return pl.ds(pl.multiple_of(block * unit, unit), unit)

    def hops(b_of, go):
        for o in range(1, a):
            zs = lax.rem(z - o + a, a)
            for u in range(half_side):
                go(o, u, zs, b_of(u))

    mine = lambda u: t * half_side + u
    other = lambda u: (1 - t) * half_side + u

    def to_line(which, value, staged):
        @pl.loop(0, side)
        def _(n):
            at = columns(n, step_n)
            part[which, :, at] = value(at)

        for j in range(a):
            staged[j] = part[which, pl.ds(j * rows, rows)].astype(BF16)

    def pre_relay(o, u, zs, b):
        place = pre_g.at[b, slot(zs)]
        arrive(place, e_ss.at[0, 0, 0], e_rs.at[0, o, u])
        send(place, place, e_ss.at[1, o, u], e_rs.at[1, o, u], pn)

    def pre_rest(o, u, zs, b):
        arrive(pre_g.at[b, slot(zs)], e_ss.at[0, 0, 0], e_rs.at[1, o, u])

    def out_relay(o, u, zs, b):
        place = lp_g.at[:, columns(zs * side + b, ff)]
        arrive(place, l_ss.at[0, 0, 0], l_rs.at[0, o, u])
        send(place, place, l_ss.at[1, o, u], l_rs.at[1, o, u], pn)

    def out_rest(o, u, zs, b):
        arrive(lp_g.at[:, columns(zs * side + b, ff)], l_ss.at[0, 0, 0], l_rs.at[1, o, u])

    def gather_late(d):
        if d < a:
            line_gather(1, late_g.at[slot(z)], late_g, d)

    def gather_early(d):
        if d < a:
            line_gather(2, early_g.at[slot(z)], early_g, d)

    def gather_cot(d):
        if d < a:
            line_gather(0, cot_g.at[slot(z)], cot_g, d)

    def sum_ig(k):
        if k < a:
            line_sum_step(0, ig_s, ig_u, ig_d, k - 1)

    def sum_lo(k):
        if k < a:
            line_sum_step(1, lo_s, lo_u, lo_d, k - 1)

    own_down.wait()
    square_send(1, down_g.at[q], down_g)
    own_cot.wait()
    gather_cot(0)
    for o in range(1, a):
        zd = lax.rem(z + o, a)
        for u in range(half_side):
            b = mine(u)
            send(early_pre.at[:, columns(zd * side + b, ff)], pre_g.at[b, slot(z)],
                 e_ss.at[0, o, u], e_rs.at[0, o, u], (zd * side + q, t))
    for copy in own_pre:
        copy.wait()
    gather_cot(1)
    square_relay(1, down_g)
    own_up.wait()
    square_send(0, up_g.at[q], up_g)
    own_late.wait()
    gather_late(0)
    gather_cot(2)
    hops(mine, pre_relay)
    for d in range(3, a):
        gather_cot(d)
    square_rest(1, down_g)
    gather_late(1)
    square_relay(0, up_g)

    @pl.loop(0, side)
    def _(b):
        gt_s[b] = dot(cot_g[...], down_g[b], 1, 1).astype(BF16)

    send(gt_s, gt_r, t_ss.at[0], t_rs.at[0], pn)
    own_early.wait()
    gather_early(0)
    hops(other, pre_rest)

    @pl.loop(0, side)
    def _(b):
        eh[b] = square_relu(pre_g[b])

    square_sum_begin(1, lambda b: dot(eh[b], cot_g[...], 0, 0), dg_s, dg_x, dg_y, dg_fx, dg_fy)
    arrive(gt_r, t_ss.at[0], t_rs.at[0])

    @pl.loop(0, side)
    def _(b):
        hidden = gt_s[b].astype(F32) + gt_r[b].astype(F32)
        pg[b] = (hidden * 2.0 * jnp.maximum(pre_g[b].astype(F32), 0.0)).astype(BF16)

    gather_late(2)
    square_rest(0, up_g)

    def ig_value(at):
        return sum(dot(pg[b], up_g[b, at, :], 1, 1) for b in range(side))

    to_line(0, ig_value, ig_s)
    sum_ig(1)
    for d in range(3, a):
        gather_late(d)

    @pl.loop(0, side)
    def _(b):
        lt_s[b] = dot(late_g[...], up_g[b], 1, 0).astype(BF16)

    send(lt_s, lt_r, t_ss.at[1], t_rs.at[1], pn)
    sum_ig(2)
    gather_early(1)
    square_sum_relay(1, dg_s, dg_x, dg_y, dg_fx, dg_fy)
    arrive(lt_r, t_ss.at[1], t_rs.at[1])

    @pl.loop(0, side)
    def _(b):
        pre = (lt_s[b].astype(F32) + lt_r[b].astype(F32)).astype(BF16)
        lp[b] = pre
        lh[b] = square_relu(pre)

    for o in range(1, a):
        zd = lax.rem(z + o, a)
        for u in range(half_side):
            b = mine(u)
            send(lp.at[b, slot(zd)], lp_g.at[:, columns(z * side + b, ff)],
                 l_ss.at[0, o, u], l_rs.at[0, o, u], (zd * side + q, t))
    for b in range(side):
        lp_g[:, columns(z * side + b, ff)] = lp[b, slot(z)]

    def lo_value(at):
        return sum(dot(lh[b], down_g[b, :, at], 1, 0) for b in range(side))

    to_line(1, lo_value, lo_s)
    sum_lo(1)
    gather_early(2)
    for k in range(3, a):
        sum_ig(k)
    sum_lo(2)
    down_v[...] = dot(eh[q], cot_g[...], 0, 0)
    for d in range(3, a):
        gather_early(d)
    square_sum_begin(0, lambda b: dot(early_g[...], pg[b], 0, 0), ug_s, ug_x, ug_y, ug_fx, ug_fy)
    up_v[...] = dot(early_g[...], pg[q], 0, 0)
    hops(mine, out_relay)
    square_sum_end(1, dg_fx, dg_fy, down_v)
    out_down = begin(down_v, down_o, 9)
    for k in range(3, a):
        sum_lo(k)
    line_sum_end(0, part.at[0], ig_u, ig_d, ig_v)
    out_ig = begin(ig_v, in_grad_o, 10)
    square_sum_relay(0, ug_s, ug_x, ug_y, ug_fx, ug_fy)
    hops(other, out_rest)
    out_pre = begin(lp_g, late_pre_o, 11)
    line_sum_end(1, part.at[1], lo_u, lo_d, lo_v)
    out_lo = begin(lo_v, late_out_o, 12)
    square_sum_end(0, ug_fx, ug_fy, up_v)
    out_up = begin(up_v, up_o, 13)

    for cond, copy in sent:
        if cond is None:
            copy.wait_send()
        else:
            pl.when(cond)(copy.wait_send)
    for copy in (out_down, out_ig, out_pre, out_lo, out_up):
        copy.wait()


def fused_body(late_input, up_weight, down_weight, early_input, early_pre, cotangent, up_sum, down_sum):
    a = lax.axis_size("fs") // 4
    side = 4
    rows, width = late_input.shape
    ff = up_weight.shape[1]
    tokens, hidden = rows * a, ff * side
    V = pltpu.VMEM
    D = pltpu.SemaphoreType.DMA
    token_block = V((tokens, width), BF16)
    hidden_block = V((side, tokens, ff), BF16)
    line_block = V((a, rows, width), BF16)
    scratch = (
        [token_block] * 3
        + [hidden_block, V((side, width, ff), BF16), V((side, ff, width), BF16)]
        + [hidden_block] * 8
        + [V((rows, hidden * a), BF16), V((2, tokens, width), F32)]
        + [line_block] * 6
        + [V((side, ff, width), BF16)] + [V((ff // 2, width), BF16)] * 2 + [V((ff, width), BF16)] * 2
        + [V((side, width, ff), BF16)] + [V((width // 2, ff), BF16)] * 2 + [V((width, ff), BF16)] * 2
        + [D((3, 2, a)), D((3, 2, a)), D((2, 2, 3)), D((2, 2, 3)), D((2, a, 2)), D((2, a, 2)),
           D((2, a, 2)), D((2, a, 2)), D((2,)), D((2,)), D((2, 2, a)), D((2, 2, a)), D((2, 6)), D((2, 6)), D((14,))]
        + [V((ff, width), F32), V((width, ff), F32)] + [V((rows, width), BF16)] * 2
    )
    flops = 12 * tokens * hidden * width
    late_pre, late_out, input_grad, up_grad, down_grad = pl.pallas_call(
        lambda *refs: fused(a, *refs),
        out_shape=(
            jax.ShapeDtypeStruct(early_pre.shape, BF16),
            jax.ShapeDtypeStruct(late_input.shape, BF16),
            jax.ShapeDtypeStruct(early_input.shape, BF16),
            jax.ShapeDtypeStruct(up_sum.shape, F32),
            jax.ShapeDtypeStruct(down_sum.shape, F32),
        ),
        in_specs=[pl.BlockSpec(memory_space=pl.ANY)] * 6,
        out_specs=[pl.BlockSpec(memory_space=pl.ANY)] * 5,
        scratch_shapes=scratch,
        compiler_params=pltpu.CompilerParams(
            collective_id=0, has_side_effects=True, vmem_limit_bytes=62 * 1024 * 1024),
        cost_estimate=pl.CostEstimate(flops=flops, bytes_accessed=1 << 24, transcendentals=0),
    )(late_input, up_weight, down_weight, early_input, early_pre, cotangent)
    return late_pre, late_out, input_grad, up_sum + up_grad, down_sum + down_grad


def contract_rows(left, right):
    return lax.dot_general(
        left, right, (((0,), (0,)), ((), ())), preferred_element_type=jnp.float32
    )


def contract_cols(left, right):
    return lax.dot_general(
        left, right, (((1,), (1,)), ((), ())), preferred_element_type=jnp.float32
    )


def body(late_input, up_weight, down_weight, early_input, early_pre, cotangent, up_sum, down_sum):
    up_gathered = lax.all_gather(up_weight, "fs", axis=1, tiled=True)
    down_gathered = lax.all_gather(down_weight, "fs", axis=0, tiled=True)
    pre_terms = jnp.dot(late_input, up_gathered, preferred_element_type=jnp.float32)
    pre_summed = lax.psum(pre_terms.astype(jnp.bfloat16), "tp")
    late_hidden = jnp.square(jax.nn.relu(pre_summed.astype(jnp.float32))).astype(jnp.bfloat16)
    early_float = early_pre.astype(jnp.float32)
    early_hidden = jnp.square(jax.nn.relu(early_float)).astype(jnp.bfloat16)
    late_out = jnp.dot(late_hidden, down_gathered, preferred_element_type=jnp.float32).astype(
        jnp.bfloat16
    )
    grad_terms = contract_cols(cotangent, down_gathered)
    hidden_grad = lax.psum(grad_terms.astype(jnp.bfloat16), "tp").astype(jnp.float32)
    pre_grad = (hidden_grad * 2.0 * jax.nn.relu(early_float)).astype(jnp.bfloat16)
    input_grad = contract_cols(pre_grad, up_gathered).astype(jnp.bfloat16)
    grad_local, hidden_local = (
        lax.all_to_all(pre_grad, "fs", split_axis=1, concat_axis=0, tiled=True),
        lax.all_to_all(early_hidden, "fs", split_axis=1, concat_axis=0, tiled=True),
    )
    rows = grad_local
    up_grad = contract_rows(lax.all_gather(early_input, "fs", axis=0, tiled=True), rows)
    up_total = up_sum + up_grad
    rows = hidden_local
    down_grad = contract_rows(rows, lax.all_gather(cotangent, "fs", axis=0, tiled=True))
    down_total = down_sum + down_grad
    return (pre_summed, late_out, input_grad, up_total, down_total)


def solution(mesh):
    in_specs = (
        P("fs", "tp"),
        P("tp", "fs"),
        P("fs", "tp"),
        P("fs", "tp"),
        P("fs", None),
        P("fs", "tp"),
        P("tp", "fs"),
        P("fs", "tp"),
    )
    out_specs = (P("fs", None), P("fs", "tp"), P("fs", "tp"), P("tp", "fs"), P("fs", "tp"))
    square_chips = mesh.shape["tp"] == 2 and mesh.shape["fs"] % 4 == 0 and mesh.shape["fs"] >= 8
    chosen = fused_body if square_chips else body
    return jax.shard_map(chosen, mesh=mesh, in_specs=in_specs, out_specs=out_specs, check_vma=False)
```
